32 devices in a mesh: fs: 8 (over z, y), tp: 4 (over x, core).
Axes of the slice: x: 2, y: 2, z: 4, core: 2. Of those that a mesh axis runs over, the one named last changes fastest.
Arguments:
- tokens: bfloat16 [4096, 2048], P('fs'), may hold values from -6 to 6
- norm_gain: float32 [2048], P('fs'), may hold values from 0.1 to 1.9
- gate_weight: float32 [2048, 6144], P('fs', 'tp'), may hold values from -0.125 to 0.125
- up_weight: float32 [2048, 6144], P('fs', 'tp'), may hold values from -0.125 to 0.125
- down_weight: float32 [6144, 2048], P('fs', 'tp'), may hold values from -0.109375 to 0.109375
Outputs:
- mixed: bfloat16 [4096, 2048], P('fs', 'tp')
- gate_out: bfloat16 [2048, 6144], P(None, 'tp')
- up_out: bfloat16 [2048, 6144], P(None, 'tp')
- down_out: bfloat16 [6144, 2048], P('tp')
The draws below stay inside these ranges and needn't reach their ends.
All inputs are finite; a program needn't handle non-finite values.
Results may differ from the reference program's by a relative error of at most 0.014.
Values may be sent and summed in bfloat16 or wider, within the bound.
A program may use at most 128 MiB of HBM per device.

```python
import jax
import jax.numpy as jnp
from jax import lax

D = 2048
FF = 6144
TOKENS = 4096
N_TP = 4


def strengthened(drawn, stream_key, source, target, blocks, factor):
    def block_of(position):
        return (jnp.arange(drawn.shape[position]) // (drawn.shape[position] // blocks)).reshape((-1,) + (1,) * (drawn.ndim - 1 - position))

    first = jax.random.permutation(stream_key, blocks)[block_of(target)]
    other_side = (block_of(target) + blocks // 2) % blocks
    return jnp.where((block_of(source) == first) | (block_of(source) == other_side), factor * drawn, drawn)


def block_levels(rng, shape, shards, least, largest):
    gain, own = 1.0, jax.random.fold_in(rng, 6)
    for position, shards_of in shards:
        heights = jnp.exp(jax.random.uniform(jax.random.fold_in(own, position), (shards_of,), jnp.float32, least / len(shards), largest / len(shards)))
        gain = gain * jnp.repeat(heights, shape[position] // shards_of).reshape([-1 if axis == position else 1 for axis in range(len(shape))])
    return gain


def noise(own_key, extent, scale, reach, pieces=(), kind=jnp.bfloat16):
    values = jax.random.normal(own_key, extent, jnp.float32) * scale
    if len(pieces) > 0:
        values = block_levels(own_key, extent, pieces, -0.22, 0.18) * values
    return jnp.clip(values, min=-reach, max=reach).astype(kind)


def bell_draw_with(rng, dims, scale, bound, cuts, heavy, held_as=jnp.bfloat16):
    array = scale * jax.random.normal(rng, dims, jnp.float32)
    if cuts:
        array = array * block_levels(rng, dims, cuts, -0.22, 0.18)
    return jnp.clip(strengthened(array, jax.random.fold_in(rng, 3), *heavy), -bound, bound).astype(held_as)


def setup_inputs(seed: int = 0) -> dict:
    key_list = jax.random.split(jax.random.key(seed), 6)
    return {
        "tokens": noise(key_list[0], (TOKENS, D), 1.0, 6.0, ((0, 8),)),
        "norm_gain": jnp.clip(1.0 + 0.18 * jax.random.normal(key_list[1], (D,), jnp.float32), 0.1, 1.9),
        "gate_weight": noise(key_list[2], (D, FF), D ** -0.5, 0.125, ((0, 8), (1, 4)), jnp.float32),
        "up_weight": noise(key_list[3], (D, FF), D ** -0.5, 0.125, ((0, 8), (1, 4)), jnp.float32),
        "down_weight": bell_draw_with(key_list[4], (FF, D), FF ** -0.5, 0.109375, ((0, 8), (1, 4)), (0, 1, 8, 2.0), jnp.float32),
    }


def reference(tokens, norm_gain, gate_weight, up_weight, down_weight):
    gate_out = (norm_gain[:, None] * gate_weight).astype(jnp.bfloat16)
    up_out = (norm_gain[:, None] * up_weight).astype(jnp.bfloat16)
    down_out = down_weight.astype(jnp.bfloat16)
    values = tokens.astype(jnp.float32)
    normed = (values * jax.lax.rsqrt(lax.optimization_barrier(jnp.mean(values * values, axis=1, keepdims=True)) + 1e-05)).astype(jnp.bfloat16)
    gate = jnp.dot(normed, gate_out, preferred_element_type=jnp.float32)
    up = jnp.dot(normed, up_out, preferred_element_type=jnp.float32)
    hidden = (jax.nn.silu(gate) * up).astype(jnp.bfloat16)
    width = FF // N_TP
    total = jnp.zeros((tokens.shape[0], D), jnp.float32)
    for block in range(N_TP):
        part = jnp.dot(hidden[:, block * width:(block + 1) * width], down_out[block * width:(block + 1) * width, :], preferred_element_type=jnp.float32)
        total = total + part.astype(jnp.bfloat16).astype(jnp.float32)
    mixed = total.astype(jnp.bfloat16)
    return (mixed, gate_out, up_out, down_out)
```

```python
import functools

import jax
import jax.numpy as jnp
from jax import lax
from jax.experimental import pallas as pl
from jax.experimental.pallas import tpu as pltpu
from jax.sharding import PartitionSpec as P

MESH = pl.DeviceIdType.MESH


def lines(fs):
    y = 1
    while 2 * (2 * y) * (2 * y) <= fs:
        y *= 2
    return fs // y, y


def gather_kernel(
    Z, Y, T, nk, nd, detour,
    g_ref, u_ref, d_ref, wg, wu, wd,
    s_up, s_dn, s_y, r_w, s_det, d_up, d_dn, d_y, r_d, s_one, r_one, s_loc,
):
    f, t = lax.axis_index("fs"), lax.axis_index("tp")
    z, y = f // Y, lax.rem(f, Y)
    has_up, has_dn = z < Z - 1, z > 0
    up, dn = (f + Y, t), (f - Y, t)
    others = [lax.rem(y + i, Y) for i in range(1, Y)]
    across = [(z * Y + o, t) for o in others]
    rows = g_ref.shape[0]
    ck = rows // nk
    rows_d, cols_d = d_ref.shape
    cd = rows_d // nd
    own, full = (g_ref, u_ref), (wg, wu)

    def when(cond, fn):
        pl.when(cond)(fn)

    barrier = pltpu.get_barrier_semaphore()

    def greet(dev):
        pl.semaphore_signal(barrier, inc=1, device_id=dev, device_id_type=MESH)

    when(has_up, lambda: greet(up))
    when(has_dn, lambda: greet(dn))
    for dev in across:
        greet(dev)
    for i in range(1, T):
        greet((f, lax.rem(t + i, T)))
    pl.semaphore_wait(barrier, Y + T - 2 + has_up.astype(jnp.int32) + has_dn.astype(jnp.int32))

    def copy(src, dst, ss, rs, dev):
        return pltpu.make_async_remote_copy(
            src_ref=src, dst_ref=dst, send_sem=ss, recv_sem=rs, device_id=dev, device_id_type=MESH
        )

    def part(a, source, k):
        return full[a].at[pl.ds(pl.multiple_of(source * rows + k * ck, ck), ck), :]

    def weight(a, k, source, ss, dev, mine=False):
        src = own[a].at[pl.ds(k * ck, ck), :] if mine else part(a, source, k)
        return copy(src, part(a, source, k), ss, r_w.at[source, a, k], dev)

    def arrived(a, k, source):
        weight(a, k, source, s_det.at[0, a, k], (f, lax.rem(t + 1, T))).wait_recv()

    pieces = [(k, a) for k in range(nk) for a in range(2)]
    sent = []

    def start(cond, make):
        sent.append((cond, make))
        if cond is None:
            make().start()
        else:
            when(cond, lambda: make().start())

    for k, a in pieces:
        start(has_up, lambda k=k, a=a: weight(a, k, f, s_up.at[z, a, k], up, True))
        start(has_dn, lambda k=k, a=a: weight(a, k, f, s_dn.at[z, a, k], dn, True))
        for i in range(Y - 1):
            start(None, lambda k=k, a=a, i=i: weight(a, k, f, s_y.at[i, z, a, k], across[i], True))

    def column(owner):
        return wd.at[
            pl.ds(pl.multiple_of(y * rows_d, rows_d), rows_d),
            pl.ds(pl.multiple_of(owner * cols_d, cols_d), cols_d),
        ]

    def first(owner, dev):
        return copy(d_ref, column(owner), s_one.at[0], r_one.at[owner], dev)

    start(z != t, lambda: first(t, (f, z)))

    locals_ = [
        pltpu.make_async_copy(
            own[a], full[a].at[pl.ds(pl.multiple_of(f * rows, rows), rows), :], s_loc.at[a]
        )
        for a in range(2)
    ]
    for c in locals_:
        c.start()
    keep = pltpu.make_async_copy(d_ref, column(t), s_loc.at[2])
    when(z == t, lambda: keep.start())

    for k, a in pieces:
        if k >= detour:
            continue
        source = across[0][0]
        arrived(a, k, source)
        start(has_up, lambda k=k, a=a, s=source: weight(a, k, s, s_det.at[0, a, k], up))
        start(has_dn, lambda k=k, a=a, s=source: weight(a, k, s, s_det.at[1, a, k], dn))

    for step in range(1, Z):
        for k, a in pieces:
            for sign in (-1, 1):
                zs = z + sign * step
                source = zs * Y + y
                valid = zs >= 0 if sign < 0 else zs < Z
                onward = jnp.logical_and(valid, has_up if sign < 0 else has_dn)
                when(valid, lambda a=a, k=k, s=source: arrived(a, k, s))
                if sign < 0:
                    start(onward, lambda a=a, k=k, s=source, q=zs: weight(a, k, s, s_up.at[q, a, k], up))
                else:
                    start(onward, lambda a=a, k=k, s=source, q=zs: weight(a, k, s, s_dn.at[q, a, k], dn))
                if step == 1 and k < detour:
                    continue
                for i in range(Y - 1):
                    start(valid, lambda a=a, k=k, s=source, q=zs, i=i: weight(a, k, s, s_y.at[i, q, a, k], across[i]))

    def rows_of(line, k):
        return wd.at[pl.ds(pl.multiple_of(line * rows_d + k * cd, cd), cd), :]

    def down(k, ss, dev, line):
        return copy(rows_of(line, k), rows_of(line, k), ss, r_d.at[line, k], dev)

    def down_arrived(k, line):
        down(k, d_up.at[k], (f, lax.rem(t + 1, T)), line).wait_recv()

    def assemble():
        keep.wait()
        for i in range(1, T):
            owner = lax.rem(t + i, T)
            first(owner, (f, owner)).wait_recv()

    when(z == t, assemble)
    go_up = jnp.logical_and(z >= t, has_up)
    go_dn = jnp.logical_and(z <= t, has_dn)
    for k in range(nd):
        when(z != t, lambda k=k: down_arrived(k, y))
        start(go_up, lambda k=k: down(k, d_up.at[k], up, y))
        start(go_dn, lambda k=k: down(k, d_dn.at[k], dn, y))
        for i in range(Y - 1):
            start(None, lambda k=k, i=i: down(k, d_y.at[i, k], across[i], y))

    for zs in range(Z):
        for o in others:
            for k, a in pieces:
                if k < detour:
                    when(zs != z, lambda a=a, k=k, zs=zs, o=o: arrived(a, k, zs * Y + o))
                else:
                    arrived(a, k, zs * Y + o)
    for o in others:
        for k in range(nd):
            down_arrived(k, o)
    for c in locals_:
        c.wait()
    for cond, make in sent:
        if cond is None:
            make().wait_send()
        else:
            when(cond, lambda make=make: make().wait_send())


def gather(mesh, g, u, d):
    fs, T = mesh.shape["fs"], mesh.shape["tp"]
    Z, Y = lines(fs)
    rows, rows_d = g.shape[0], d.shape[0]
    nk = max(1, min(4, rows // 64))
    nd = max(1, min(8, rows_d // 96))
    detour = nk // 2 if Y == 2 else 0
    dma = pltpu.SemaphoreType.DMA
    any_ = pl.BlockSpec(memory_space=pl.ANY)
    return pl.pallas_call(
        functools.partial(gather_kernel, Z, Y, T, nk, nd, detour),
        out_shape=(
            jax.ShapeDtypeStruct((rows * fs, g.shape[1]), g.dtype),
            jax.ShapeDtypeStruct((rows * fs, g.shape[1]), g.dtype),
            jax.ShapeDtypeStruct((rows_d * Y, d.shape[1] * T), d.dtype),
        ),
        in_specs=[any_] * 3,
        out_specs=[any_] * 3,
        scratch_shapes=[
            dma((Z, 2, nk)), dma((Z, 2, nk)), dma((max(Y - 1, 1), Z, 2, nk)), dma((fs, 2, nk)),
            dma((2, 2, nk)), dma((nd,)), dma((nd,)), dma((max(Y - 1, 1), nd)), dma((Y, nd)),
            dma((1,)), dma((T,)), dma((3,)),
        ],
        compiler_params=pltpu.CompilerParams(collective_id=0, has_side_effects=True),
        name="gather",
    )(g, u, d)


def layer_kernel(x_ref, wg, wu, wd, part, og, ou, od, normed, total):
    j = pl.program_id(0)

    @pl.when(j == 0)
    def _():
        v = x_ref[...].astype(jnp.float32)
        normed[...] = (v * lax.rsqrt(jnp.mean(v * v, axis=1, keepdims=True) + 1e-05)).astype(jnp.bfloat16)
        total[...] = jnp.zeros_like(total)

    og[...] = wg[...]
    ou[...] = wu[...]
    od[...] = wd[...]
    gate = jnp.dot(normed[...], wg[...], preferred_element_type=jnp.float32)
    up = jnp.dot(normed[...], wu[...], preferred_element_type=jnp.float32)
    hidden = (gate / (1.0 + jnp.exp(-gate)) * up).astype(jnp.bfloat16)
    total[...] += jnp.dot(hidden, wd[...], preferred_element_type=jnp.float32)

    @pl.when(j == pl.num_programs(0) - 1)
    def _():
        part[...] = total[...].astype(jnp.bfloat16)


def layer(x, wg, wu, wd):
    n, depth = x.shape
    units = wg.shape[1]
    width = 256 if units % 256 == 0 else 128
    spec_w = pl.BlockSpec((depth, width), lambda j: (0, j))
    spec_d = pl.BlockSpec((width, wd.shape[1]), lambda j: (j, 0))
    whole = pl.BlockSpec((n, depth), lambda j: (0, 0))
    return pl.pallas_call(
        layer_kernel,
        grid=(units // width,),
        out_shape=(
            jax.ShapeDtypeStruct((n, wd.shape[1]), jnp.bfloat16),
            jax.ShapeDtypeStruct(wg.shape, wg.dtype),
            jax.ShapeDtypeStruct(wu.shape, wu.dtype),
            jax.ShapeDtypeStruct(wd.shape, wd.dtype),
        ),
        in_specs=[whole, spec_w, spec_w, spec_d],
        out_specs=[pl.BlockSpec((n, wd.shape[1]), lambda j: (0, 0)), spec_w, spec_w, spec_d],
        scratch_shapes=[
            pltpu.VMEM((n, depth), jnp.bfloat16),
            pltpu.VMEM((n, wd.shape[1]), jnp.float32),
        ],
        compiler_params=pltpu.CompilerParams(vmem_limit_bytes=60 * 1024 * 1024),
        name="layer",
    )(x, wg, wu, wd)


def sum_kernel(X, nc, p_ref, o_ref, near, pair, far, s_a, r_a, s_b, r_b):
    f, t = lax.axis_index("fs"), lax.axis_index("tp")
    x, core = t // 2, lax.rem(t, 2)
    mate = (f, x * 2 + 1 - core)
    n, width = o_ref.shape
    h = n // nc
    barrier = pltpu.get_barrier_semaphore()
    xs = [lax.rem(x + i, X) for i in range(1, X)]
    peers = [mate] + [(f, q * 2 + core) for q in xs]
    for dev in peers:
        pl.semaphore_signal(barrier, inc=1, device_id=dev, device_id_type=MESH)
    pl.semaphore_wait(barrier, len(peers))

    order = [(c, i) for c in range(nc) for i in list(range(1, X)) + [0]]

    def block(c, i, which):
        q = lax.rem(x + i, X)
        start = pl.multiple_of((q * 2 + which) * width, width)
        return p_ref.at[pl.ds(c * h, h), pl.ds(start, width)]

    def to_mate(c, i):
        return pltpu.make_async_remote_copy(
            src_ref=block(c, i, 1 - core), dst_ref=near.at[i, pl.ds(c * h, h), :],
            send_sem=s_a.at[i, c], recv_sem=r_a.at[i, c], device_id=mate, device_id_type=MESH,
        )

    def to_far(c, i):
        return pltpu.make_async_remote_copy(
            src_ref=pair.at[i, pl.ds(c * h, h), :], dst_ref=far.at[i, pl.ds(c * h, h), :],
            send_sem=s_b.at[i, c], recv_sem=r_b.at[i, c], device_id=peers[i], device_id_type=MESH,
        )

    order = [(c, i) for c in range(nc) for i in range(1, X)]
    for c, i in order:
        to_mate(c, i).start()
    for c in range(nc):
        to_mate(c, 0).start()
    for c, i in order:
        to_mate(c, i).wait_recv()
        pair[i, pl.ds(c * h, h), :] = (
            block(c, i, core)[...].astype(jnp.float32) + near[i, pl.ds(c * h, h), :].astype(jnp.float32)
        ).astype(jnp.bfloat16)
        to_far(c, i).start()
    for c in range(nc):
        to_mate(c, 0).wait_recv()
        acc = block(c, 0, core)[...].astype(jnp.float32) + near[0, pl.ds(c * h, h), :].astype(jnp.float32)
        for i in range(1, X):
            to_far(c, i).wait_recv()
            acc = acc + far[i, pl.ds(c * h, h), :].astype(jnp.float32)
        o_ref[pl.ds(c * h, h), :] = acc.astype(o_ref.dtype)
    for c in range(nc):
        for i in range(X):
            to_mate(c, i).wait_send()
            if i:
                to_far(c, i).wait_send()


def sum_parts(mesh, p):
    T = mesh.shape["tp"]
    X = T // 2
    n, width = p.shape[0], p.shape[1] // T
    nc = 4
    dma = pltpu.SemaphoreType.DMA
    vmem = pl.BlockSpec(memory_space=pltpu.VMEM)
    return pl.pallas_call(
        functools.partial(sum_kernel, X, nc),
        out_shape=jax.ShapeDtypeStruct((n, width), jnp.bfloat16),
        in_specs=[vmem],
        out_specs=vmem,
        scratch_shapes=[pltpu.VMEM((X, n, width), jnp.bfloat16)] * 3 + [dma((X, nc))] * 4,
        compiler_params=pltpu.CompilerParams(
            collective_id=1, has_side_effects=True, vmem_limit_bytes=48 * 1024 * 1024
        ),
        name="sum_parts",
    )(p)


def solution(mesh):
    def on_device(tokens, norm_gain, gate_weight, up_weight, down_weight):
        row_gain = norm_gain[:, None]
        gate_local = (row_gain * gate_weight).astype(jnp.bfloat16)
        up_local = (row_gain * up_weight).astype(jnp.bfloat16)
        down_local = down_weight.astype(jnp.bfloat16)
        wg, wu, wd = gather(mesh, gate_local, up_local, down_local)
        part, og, ou, od = layer(tokens, wg, wu, wd)
        return (sum_parts(mesh, part), og, ou, od)

    return jax.shard_map(
        on_device,
        mesh=mesh,
        in_specs=(P("fs", None), P("fs"), P("fs", "tp"), P("fs", "tp"), P("fs", "tp")),
        out_specs=(P("fs", "tp"), P(None, "tp"), P(None, "tp"), P("tp", None)),
        check_vma=False,
    )
```

```python
import functools

import jax
import jax.numpy as jnp
from jax import lax
from jax.experimental import pallas as pl
from jax.experimental.pallas import tpu as pltpu
from jax.sharding import PartitionSpec as P

MESH = pl.DeviceIdType.MESH
GRANT = 16 * 1024 * 1024


def lines(fs):
    y = 1
    while 2 * (2 * y) * (2 * y) <= fs:
        y *= 2
    return fs // y, y


def gather_kernel(
    Z, Y, T, nk, nd, detour,
    g_ref, u_ref, d_ref, x_ref, wg, wu, wd, hidden,
    normed, s_up, s_dn, s_y, r_w, s_det, d_up, d_dn, d_y, r_d, s_one, r_one,
):
    f, t = lax.axis_index("fs"), lax.axis_index("tp")
    z, y = f // Y, lax.rem(f, Y)
    has_up, has_dn = z < Z - 1, z > 0
    up, dn = (f + Y, t), (f - Y, t)
    others = [lax.rem(y + i, Y) for i in range(1, Y)]
    across = [(z * Y + o, t) for o in others]
    rows = g_ref.shape[0]
    ck = rows // nk
    rows_d, cols_d = d_ref.shape
    cd = rows_d // nd
    own, full = (g_ref, u_ref), (wg, wu)

    def when(cond, fn):
        pl.when(cond)(fn)

    barrier = pltpu.get_barrier_semaphore()

    def greet(dev):
        pl.semaphore_signal(barrier, inc=1, device_id=dev, device_id_type=MESH)

    when(has_up, lambda: greet(up))
    when(has_dn, lambda: greet(dn))
    for dev in across:
        greet(dev)
    for i in range(1, T):
        greet((f, lax.rem(t + i, T)))
    pl.semaphore_wait(barrier, Y + T - 2 + has_up.astype(jnp.int32) + has_dn.astype(jnp.int32))

    def copy(src, dst, ss, rs, dev):
        return pltpu.make_async_remote_copy(
            src_ref=src, dst_ref=dst, send_sem=ss, recv_sem=rs, device_id=dev, device_id_type=MESH
        )

    def part(a, source, k):
        return full[a].at[pl.ds(pl.multiple_of(source * rows + k * ck, ck), ck), :]

    def weight(a, k, source, ss, dev, mine=False):
        src = own[a].at[pl.ds(k * ck, ck), :] if mine else part(a, source, k)
        return copy(src, part(a, source, k), ss, r_w.at[source, a, k], dev)

    def arrived(a, k, source):
        weight(a, k, source, s_det.at[0, a, k], (f, lax.rem(t + 1, T))).wait_recv()

    pieces = [(k, a) for k in range(nk) for a in range(2)]
    sent = []

    def start(cond, make):
        sent.append((cond, make))
        if cond is None:
            make().start()
        else:
            when(cond, lambda: make().start())

    for k, a in pieces:
        start(has_up, lambda k=k, a=a: weight(a, k, f, s_up.at[z, a, k], up, True))
        start(has_dn, lambda k=k, a=a: weight(a, k, f, s_dn.at[z, a, k], dn, True))
        for i in range(Y - 1):
            start(None, lambda k=k, a=a, i=i: weight(a, k, f, s_y.at[i, z, a, k], across[i], True))

    def column(owner):
        return wd.at[
            pl.ds(pl.multiple_of(y * rows_d, rows_d), rows_d),
            pl.ds(pl.multiple_of(owner * cols_d, cols_d), cols_d),
        ]

    def first(owner, dev):
        return copy(d_ref, column(owner), s_one.at[0], r_one.at[owner], dev)

    start(z != t, lambda: first(t, (f, z)))

    for a in range(2):
        full[a][pl.ds(pl.multiple_of(f * rows, rows), rows), :] = own[a][...]

    def keep():
        wd[
            pl.ds(pl.multiple_of(y * rows_d, rows_d), rows_d),
            pl.ds(pl.multiple_of(t * cols_d, cols_d), cols_d),
        ] = d_ref[...]

    when(z == t, keep)

    n = x_ref.shape[0]
    slab = 64 if n % 64 == 0 else n

    @pl.loop(0, n // slab)
    def _(i):
        at = pl.ds(pl.multiple_of(i * slab, slab), slab)
        v = x_ref[at, :].astype(jnp.float32)
        normed[at, :] = (v * lax.rsqrt(jnp.mean(v * v, axis=1, keepdims=True) + 1e-05)).astype(jnp.bfloat16)

    for k, a in pieces:
        if k >= detour:
            continue
        source = across[0][0]
        arrived(a, k, source)
        start(has_up, lambda k=k, a=a, s=source: weight(a, k, s, s_det.at[0, a, k], up))
        start(has_dn, lambda k=k, a=a, s=source: weight(a, k, s, s_det.at[1, a, k], dn))

    for step in range(1, Z):
        for k, a in pieces:
            for sign in (-1, 1):
                zs = z + sign * step
                source = zs * Y + y
                valid = zs >= 0 if sign < 0 else zs < Z
                onward = jnp.logical_and(valid, has_up if sign < 0 else has_dn)
                when(valid, lambda a=a, k=k, s=source: arrived(a, k, s))
                if sign < 0:
                    start(onward, lambda a=a, k=k, s=source, q=zs: weight(a, k, s, s_up.at[q, a, k], up))
                else:
                    start(onward, lambda a=a, k=k, s=source, q=zs: weight(a, k, s, s_dn.at[q, a, k], dn))
                if step == 1 and k < detour:
                    continue
                for i in range(Y - 1):
                    start(valid, lambda a=a, k=k, s=source, q=zs, i=i: weight(a, k, s, s_y.at[i, q, a, k], across[i]))

    def rows_of(line, k):
        return wd.at[pl.ds(pl.multiple_of(line * rows_d + k * cd, cd), cd), :]

    def down(k, ss, dev, line):
        return copy(rows_of(line, k), rows_of(line, k), ss, r_d.at[line, k], dev)

    def down_arrived(k, line):
        down(k, d_up.at[k], (f, lax.rem(t + 1, T)), line).wait_recv()

    def assemble():
        for i in range(1, T):
            owner = lax.rem(t + i, T)
            first(owner, (f, owner)).wait_recv()

    when(z == t, assemble)
    go_up = jnp.logical_and(z >= t, has_up)
    go_dn = jnp.logical_and(z <= t, has_dn)
    for k in range(nd):
        when(z != t, lambda k=k: down_arrived(k, y))
        start(go_up, lambda k=k: down(k, d_up.at[k], up, y))
        start(go_dn, lambda k=k: down(k, d_dn.at[k], dn, y))
        for i in range(Y - 1):
            start(None, lambda k=k, i=i: down(k, d_y.at[i, k], across[i], y))

    for zs in range(Z):
        for o in others:
            for k, a in pieces:
                if k < detour:
                    when(zs != z, lambda a=a, k=k, zs=zs, o=o: arrived(a, k, zs * Y + o))
                else:
                    arrived(a, k, zs * Y + o)
    units = wg.shape[1]
    width = 256 if units % 256 == 0 else 128

    @pl.loop(0, units // width)
    def _(j):
        at = pl.ds(pl.multiple_of(j * width, width), width)
        gate = jnp.dot(normed[...], wg[:, at], preferred_element_type=jnp.float32)
        up_ = jnp.dot(normed[...], wu[:, at], preferred_element_type=jnp.float32)
        hidden[:, at] = (gate / (1.0 + jnp.exp(-gate)) * up_).astype(jnp.bfloat16)

    for o in others:
        for k in range(nd):
            down_arrived(k, o)
    for cond, make in sent:
        if cond is None:
            make().wait_send()
        else:
            when(cond, lambda make=make: make().wait_send())


def gather(mesh, g, u, d, x):
    fs, T = mesh.shape["fs"], mesh.shape["tp"]
    Z, Y = lines(fs)
    rows, rows_d = g.shape[0], d.shape[0]
    nk = max(1, min(4, rows // 64))
    nd = max(1, min(8, rows_d // 96))
    detour = nk // 2 if Y == 2 else 0
    dma = pltpu.SemaphoreType.DMA
    vmem = pl.BlockSpec(memory_space=pltpu.VMEM)
    return pl.pallas_call(
        functools.partial(gather_kernel, Z, Y, T, nk, nd, detour),
        out_shape=(
            jax.ShapeDtypeStruct((rows * fs, g.shape[1]), g.dtype),
            jax.ShapeDtypeStruct((rows * fs, g.shape[1]), g.dtype),
            jax.ShapeDtypeStruct((rows_d * Y, d.shape[1] * T), d.dtype),
            jax.ShapeDtypeStruct((x.shape[0], g.shape[1]), d.dtype),
        ),
        in_specs=[vmem] * 4,
        out_specs=[vmem] * 4,
        scratch_shapes=[
            pltpu.VMEM(x.shape, x.dtype),
            dma((Z, 2, nk)), dma((Z, 2, nk)), dma((max(Y - 1, 1), Z, 2, nk)), dma((fs, 2, nk)),
            dma((2, 2, nk)), dma((nd,)), dma((nd,)), dma((max(Y - 1, 1), nd)), dma((Y, nd)),
            dma((1,)), dma((T,)),
        ],
        compiler_params=pltpu.CompilerParams(
            collective_id=0, has_side_effects=True, vmem_limit_bytes=GRANT
        ),
        name="gather",
    )(g, u, d, x)


def layer_kernel(T, h_ref, wg, wu, wd, part, og, ou, od, sems):
    outs = [pltpu.make_async_copy(s, d, sems.at[i]) for i, (s, d) in enumerate(((wg, og), (wu, ou), (wd, od)))]
    for c in outs:
        c.start()
    width = part.shape[1] // T

    @pl.loop(0, T)
    def _(j):
        at = pl.ds(pl.multiple_of(j * width, width), width)
        part[:, at] = jnp.dot(h_ref[...], wd[:, at], preferred_element_type=jnp.float32).astype(jnp.bfloat16)

    for c in outs:
        c.wait()


def layer(mesh, h, wg, wu, wd):
    vmem, any_ = pl.BlockSpec(memory_space=pltpu.VMEM), pl.BlockSpec(memory_space=pl.ANY)
    return pl.pallas_call(
        functools.partial(layer_kernel, mesh.shape["tp"]),
        out_shape=(
            jax.ShapeDtypeStruct((h.shape[0], wd.shape[1]), jnp.bfloat16),
            jax.ShapeDtypeStruct(wg.shape, wg.dtype),
            jax.ShapeDtypeStruct(wu.shape, wu.dtype),
            jax.ShapeDtypeStruct(wd.shape, wd.dtype),
        ),
        in_specs=[vmem] * 4,
        out_specs=[vmem] + [any_] * 3,
        scratch_shapes=[pltpu.SemaphoreType.DMA((3,))],
        compiler_params=pltpu.CompilerParams(vmem_limit_bytes=GRANT),
        name="layer",
    )(h, wg, wu, wd)


def sum_kernel(X, nc, p_ref, o_ref, near, pair, far, s_a, r_a, s_b, r_b):
    f, t = lax.axis_index("fs"), lax.axis_index("tp")
    x, core = t // 2, lax.rem(t, 2)
    mate = (f, x * 2 + 1 - core)
    n, width = o_ref.shape
    h = n // nc
    barrier = pltpu.get_barrier_semaphore()
    xs = [lax.rem(x + i, X) for i in range(1, X)]
    peers = [mate] + [(f, q * 2 + core) for q in xs]
    for dev in peers:
        pl.semaphore_signal(barrier, inc=1, device_id=dev, device_id_type=MESH)
    pl.semaphore_wait(barrier, len(peers))

    order = [(c, i) for c in range(nc) for i in list(range(1, X)) + [0]]

    def block(c, i, which):
        q = lax.rem(x + i, X)
        start = pl.multiple_of((q * 2 + which) * width, width)
        return p_ref.at[pl.ds(c * h, h), pl.ds(start, width)]

    def to_mate(c, i):
        return pltpu.make_async_remote_copy(
            src_ref=block(c, i, 1 - core), dst_ref=near.at[i, pl.ds(c * h, h), :],
            send_sem=s_a.at[i, c], recv_sem=r_a.at[i, c], device_id=mate, device_id_type=MESH,
        )

    def to_far(c, i):
        return pltpu.make_async_remote_copy(
            src_ref=pair.at[i, pl.ds(c * h, h), :], dst_ref=far.at[i, pl.ds(c * h, h), :],
            send_sem=s_b.at[i, c], recv_sem=r_b.at[i, c], device_id=peers[i], device_id_type=MESH,
        )

    order = [(c, i) for c in range(nc) for i in range(1, X)]
    for c, i in order:
        to_mate(c, i).start()
    for c in range(nc):
        to_mate(c, 0).start()
    for c, i in order:
        to_mate(c, i).wait_recv()
        pair[i, pl.ds(c * h, h), :] = (
            block(c, i, core)[...].astype(jnp.float32) + near[i, pl.ds(c * h, h), :].astype(jnp.float32)
        ).astype(jnp.bfloat16)
        to_far(c, i).start()
    for c in range(nc):
        to_mate(c, 0).wait_recv()
        acc = block(c, 0, core)[...].astype(jnp.float32) + near[0, pl.ds(c * h, h), :].astype(jnp.float32)
        for i in range(1, X):
            to_far(c, i).wait_recv()
            acc = acc + far[i, pl.ds(c * h, h), :].astype(jnp.float32)
        o_ref[pl.ds(c * h, h), :] = acc.astype(o_ref.dtype)
    for c in range(nc):
        for i in range(X):
            to_mate(c, i).wait_send()
            if i:
                to_far(c, i).wait_send()


def sum_parts(mesh, p):
    T = mesh.shape["tp"]
    X = T // 2
    n, width = p.shape[0], p.shape[1] // T
    nc = 4
    dma = pltpu.SemaphoreType.DMA
    vmem = pl.BlockSpec(memory_space=pltpu.VMEM)
    return pl.pallas_call(
        functools.partial(sum_kernel, X, nc),
        out_shape=jax.ShapeDtypeStruct((n, width), jnp.bfloat16),
        in_specs=[vmem],
        out_specs=vmem,
        scratch_shapes=[pltpu.VMEM((X, n, width), jnp.bfloat16)] * 3 + [dma((X, nc))] * 4,
        compiler_params=pltpu.CompilerParams(
            collective_id=1, has_side_effects=True, vmem_limit_bytes=16 * 1024 * 1024
        ),
        name="sum_parts",
    )(p)


def solution(mesh):
    def on_device(tokens, norm_gain, gate_weight, up_weight, down_weight):
        row_gain = norm_gain[:, None]
        gate_local = (row_gain * gate_weight).astype(jnp.bfloat16)
        up_local = (row_gain * up_weight).astype(jnp.bfloat16)
        down_local = down_weight.astype(jnp.bfloat16)
        wg, wu, wd, hidden = gather(mesh, gate_local, up_local, down_local, tokens)
        part, og, ou, od = layer(mesh, hidden, wg, wu, wd)
        return (sum_parts(mesh, part), og, ou, od)

    return jax.shard_map(
        on_device,
        mesh=mesh,
        in_specs=(P("fs", None), P("fs"), P("fs", "tp"), P("fs", "tp"), P("fs", "tp")),
        out_specs=(P("fs", "tp"), P(None, "tp"), P(None, "tp"), P("tp", None)),
        check_vma=False,
    )
```

```python
import functools

import jax
import jax.numpy as jnp
from jax import lax
from jax.experimental import pallas as pl
from jax.experimental.pallas import tpu as pltpu
from jax.sharding import PartitionSpec as P

MESH = pl.DeviceIdType.MESH
GRANT = 16 * 1024 * 1024


def lines(fs):
    y = 1
    while 2 * (2 * y) * (2 * y) <= fs:
        y *= 2
    return fs // y, y


def gather_kernel(
    Z, Y, T, nk, nd, detour,
    g_ref, u_ref, d_ref, x_ref, wg, wu, wd, hidden,
    normed, s_up, s_dn, s_y, r_w, s_det, d_up, d_dn, d_y, r_d, s_one, r_one,
):
    f, t = lax.axis_index("fs"), lax.axis_index("tp")
    z, y = f // Y, lax.rem(f, Y)
    has_up, has_dn = z < Z - 1, z > 0
    up, dn = (f + Y, t), (f - Y, t)
    others = [lax.rem(y + i, Y) for i in range(1, Y)]
    across = [(z * Y + o, t) for o in others]
    rows = g_ref.shape[0]
    ck = rows // nk
    rows_d, cols_d = d_ref.shape
    cd = rows_d // nd
    own, full = (g_ref, u_ref), (wg, wu)

    def when(cond, fn):
        pl.when(cond)(fn)

    barrier = pltpu.get_barrier_semaphore()

    def greet(dev):
        pl.semaphore_signal(barrier, inc=1, device_id=dev, device_id_type=MESH)

    when(has_up, lambda: greet(up))
    when(has_dn, lambda: greet(dn))
    for dev in across:
        greet(dev)
    for i in range(1, T):
        greet((f, lax.rem(t + i, T)))
    pl.semaphore_wait(barrier, Y + T - 2 + has_up.astype(jnp.int32) + has_dn.astype(jnp.int32))

    def copy(src, dst, ss, rs, dev):
        return pltpu.make_async_remote_copy(
            src_ref=src, dst_ref=dst, send_sem=ss, recv_sem=rs, device_id=dev, device_id_type=MESH
        )

    def part(a, source, k):
        return full[a].at[pl.ds(pl.multiple_of(source * rows + k * ck, ck), ck), :]

    def weight(a, k, source, ss, dev, mine=False):
        src = own[a].at[pl.ds(k * ck, ck), :] if mine else part(a, source, k)
        return copy(src, part(a, source, k), ss, r_w.at[source, a, k], dev)

    def arrived(a, k, source):
        weight(a, k, source, s_det.at[0, a, k], (f, lax.rem(t + 1, T))).wait_recv()

    pieces = [(k, a) for k in range(nk) for a in range(2)]
    sent = []

    def start(cond, make):
        sent.append((cond, make))
        if cond is None:
            make().start()
        else:
            when(cond, lambda: make().start())

    for k, a in pieces:
        start(has_up, lambda k=k, a=a: weight(a, k, f, s_up.at[z, a, k], up, True))
        start(has_dn, lambda k=k, a=a: weight(a, k, f, s_dn.at[z, a, k], dn, True))
        for i in range(Y - 1):
            start(None, lambda k=k, a=a, i=i: weight(a, k, f, s_y.at[i, z, a, k], across[i], True))

    def column(owner):
        return wd.at[
            pl.ds(pl.multiple_of(y * rows_d, rows_d), rows_d),
            pl.ds(pl.multiple_of(owner * cols_d, cols_d), cols_d),
        ]

    def first(owner, dev):
        return copy(d_ref, column(owner), s_one.at[0], r_one.at[owner], dev)

    start(z != t, lambda: first(t, (f, z)))

    for a in range(2):
        full[a][pl.ds(pl.multiple_of(f * rows, rows), rows), :] = own[a][...]

    def keep():
        wd[
            pl.ds(pl.multiple_of(y * rows_d, rows_d), rows_d),
            pl.ds(pl.multiple_of(t * cols_d, cols_d), cols_d),
        ] = d_ref[...]

    when(z == t, keep)

    n = x_ref.shape[0]
    slab = 64 if n % 64 == 0 else n

    @pl.loop(0, n // slab)
    def _(i):
        at = pl.ds(pl.multiple_of(i * slab, slab), slab)
        v = x_ref[at, :].astype(jnp.float32)
        normed[at, :] = (v * lax.rsqrt(jnp.mean(v * v, axis=1, keepdims=True) + 1e-05)).astype(jnp.bfloat16)

    for k, a in pieces:
        if k >= detour:
            continue
        source = across[0][0]
        arrived(a, k, source)
        start(has_up, lambda k=k, a=a, s=source: weight(a, k, s, s_det.at[0, a, k], up))
        start(has_dn, lambda k=k, a=a, s=source: weight(a, k, s, s_det.at[1, a, k], dn))

    for step in range(1, Z):
        for k, a in pieces:
            for sign in (-1, 1):
                zs = z + sign * step
                source = zs * Y + y
                valid = zs >= 0 if sign < 0 else zs < Z
                onward = jnp.logical_and(valid, has_up if sign < 0 else has_dn)
                when(valid, lambda a=a, k=k, s=source: arrived(a, k, s))
                if sign < 0:
                    start(onward, lambda a=a, k=k, s=source, q=zs: weight(a, k, s, s_up.at[q, a, k], up))
                else:
                    start(onward, lambda a=a, k=k, s=source, q=zs: weight(a, k, s, s_dn.at[q, a, k], dn))
                if step == 1 and k < detour:
                    continue
                for i in range(Y - 1):
                    start(valid, lambda a=a, k=k, s=source, q=zs, i=i: weight(a, k, s, s_y.at[i, q, a, k], across[i]))

    def rows_of(line, k):
        return wd.at[pl.ds(pl.multiple_of(line * rows_d + k * cd, cd), cd), :]

    def down(k, ss, dev, line):
        return copy(rows_of(line, k), rows_of(line, k), ss, r_d.at[line, k], dev)

    def down_arrived(k, line):
        down(k, d_up.at[k], (f, lax.rem(t + 1, T)), line).wait_recv()

    def assemble():
        for i in range(1, T):
            owner = lax.rem(t + i, T)
            first(owner, (f, owner)).wait_recv()

    when(z == t, assemble)
    go_up = jnp.logical_and(z >= t, has_up)
    go_dn = jnp.logical_and(z <= t, has_dn)
    for k in range(nd):
        when(z != t, lambda k=k: down_arrived(k, y))
        start(go_up, lambda k=k: down(k, d_up.at[k], up, y))
        start(go_dn, lambda k=k: down(k, d_dn.at[k], dn, y))
        for i in range(Y - 1):
            start(None, lambda k=k, i=i: down(k, d_y.at[i, k], across[i], y))

    for zs in range(Z):
        for o in others:
            for k, a in pieces:
                if k < detour:
                    when(zs != z, lambda a=a, k=k, zs=zs, o=o: arrived(a, k, zs * Y + o))
                else:
                    arrived(a, k, zs * Y + o)
    units = wg.shape[1]
    width = 256 if units % 256 == 0 else 128

    @pl.loop(0, units // width)
    def _(j):
        at = pl.ds(pl.multiple_of(j * width, width), width)
        gate = jnp.dot(normed[...], wg[:, at], preferred_element_type=jnp.float32)
        up_ = jnp.dot(normed[...], wu[:, at], preferred_element_type=jnp.float32)
        hidden[:, at] = (gate / (1.0 + jnp.exp(-gate)) * up_).astype(jnp.bfloat16)

    for o in others:
        for k in range(nd):
            down_arrived(k, o)
    for cond, make in sent:
        if cond is None:
            make().wait_send()
        else:
            when(cond, lambda make=make: make().wait_send())


def gather(mesh, g, u, d, x):
    fs, T = mesh.shape["fs"], mesh.shape["tp"]
    Z, Y = lines(fs)
    rows, rows_d = g.shape[0], d.shape[0]
    nk = max(1, min(4, rows // 64))
    nd = max(1, min(16, rows_d // 48))
    detour = nk // 2 if Y == 2 else 0
    dma = pltpu.SemaphoreType.DMA
    vmem = pl.BlockSpec(memory_space=pltpu.VMEM)
    return pl.pallas_call(
        functools.partial(gather_kernel, Z, Y, T, nk, nd, detour),
        out_shape=(
            jax.ShapeDtypeStruct((rows * fs, g.shape[1]), g.dtype),
            jax.ShapeDtypeStruct((rows * fs, g.shape[1]), g.dtype),
            jax.ShapeDtypeStruct((rows_d * Y, d.shape[1] * T), d.dtype),
            jax.ShapeDtypeStruct((x.shape[0], g.shape[1]), d.dtype),
        ),
        in_specs=[vmem] * 4,
        out_specs=[vmem] * 4,
        scratch_shapes=[
            pltpu.VMEM(x.shape, x.dtype),
            dma((Z, 2, nk)), dma((Z, 2, nk)), dma((max(Y - 1, 1), Z, 2, nk)), dma((fs, 2, nk)),
            dma((2, 2, nk)), dma((nd,)), dma((nd,)), dma((max(Y - 1, 1), nd)), dma((Y, nd)),
            dma((1,)), dma((T,)),
        ],
        compiler_params=pltpu.CompilerParams(
            collective_id=0, has_side_effects=True, vmem_limit_bytes=GRANT
        ),
        name="gather",
    )(g, u, d, x)


def layer_kernel(T, h_ref, wg, wu, wd, part, og, ou, od, sems):
    outs = [pltpu.make_async_copy(s, d, sems.at[i]) for i, (s, d) in enumerate(((wg, og), (wu, ou), (wd, od)))]
    for c in outs:
        c.start()
    width = part.shape[1] // T

    @pl.loop(0, T)
    def _(j):
        at = pl.ds(pl.multiple_of(j * width, width), width)
        part[:, at] = jnp.dot(h_ref[...], wd[:, at], preferred_element_type=jnp.float32).astype(jnp.bfloat16)

    for c in outs:
        c.wait()


def layer(mesh, h, wg, wu, wd):
    vmem, any_ = pl.BlockSpec(memory_space=pltpu.VMEM), pl.BlockSpec(memory_space=pl.ANY)
    return pl.pallas_call(
        functools.partial(layer_kernel, mesh.shape["tp"]),
        out_shape=(
            jax.ShapeDtypeStruct((h.shape[0], wd.shape[1]), jnp.bfloat16),
            jax.ShapeDtypeStruct(wg.shape, wg.dtype),
            jax.ShapeDtypeStruct(wu.shape, wu.dtype),
            jax.ShapeDtypeStruct(wd.shape, wd.dtype),
        ),
        in_specs=[vmem] * 4,
        out_specs=[vmem] + [any_] * 3,
        scratch_shapes=[pltpu.SemaphoreType.DMA((3,))],
        compiler_params=pltpu.CompilerParams(vmem_limit_bytes=GRANT),
        name="layer",
    )(h, wg, wu, wd)


def sum_kernel(X, nc, p_ref, o_ref, near, pair, far, s_a, r_a, s_b, r_b):
    f, t = lax.axis_index("fs"), lax.axis_index("tp")
    x, core = t // 2, lax.rem(t, 2)
    mate = (f, x * 2 + 1 - core)
    n, width = o_ref.shape
    h = n // nc
    barrier = pltpu.get_barrier_semaphore()
    xs = [lax.rem(x + i, X) for i in range(1, X)]
    peers = [mate] + [(f, q * 2 + core) for q in xs]
    for dev in peers:
        pl.semaphore_signal(barrier, inc=1, device_id=dev, device_id_type=MESH)
    pl.semaphore_wait(barrier, len(peers))

    order = [(c, i) for c in range(nc) for i in list(range(1, X)) + [0]]

    def block(c, i, which):
        q = lax.rem(x + i, X)
        start = pl.multiple_of((q * 2 + which) * width, width)
        return p_ref.at[pl.ds(c * h, h), pl.ds(start, width)]

    def to_mate(c, i):
        return pltpu.make_async_remote_copy(
            src_ref=block(c, i, 1 - core), dst_ref=near.at[i, pl.ds(c * h, h), :],
            send_sem=s_a.at[i, c], recv_sem=r_a.at[i, c], device_id=mate, device_id_type=MESH,
        )

    def to_far(c, i):
        return pltpu.make_async_remote_copy(
            src_ref=pair.at[i, pl.ds(c * h, h), :], dst_ref=far.at[i, pl.ds(c * h, h), :],
            send_sem=s_b.at[i, c], recv_sem=r_b.at[i, c], device_id=peers[i], device_id_type=MESH,
        )

    order = [(c, i) for c in range(nc) for i in range(1, X)]
    for c, i in order:
        to_mate(c, i).start()
    for c in range(nc):
        to_mate(c, 0).start()
    for c, i in order:
        to_mate(c, i).wait_recv()
        pair[i, pl.ds(c * h, h), :] = (
            block(c, i, core)[...].astype(jnp.float32) + near[i, pl.ds(c * h, h), :].astype(jnp.float32)
        ).astype(jnp.bfloat16)
        to_far(c, i).start()
    for c in range(nc):
        to_mate(c, 0).wait_recv()
        acc = block(c, 0, core)[...].astype(jnp.float32) + near[0, pl.ds(c * h, h), :].astype(jnp.float32)
        for i in range(1, X):
            to_far(c, i).wait_recv()
            acc = acc + far[i, pl.ds(c * h, h), :].astype(jnp.float32)
        o_ref[pl.ds(c * h, h), :] = acc.astype(o_ref.dtype)
    for c in range(nc):
        for i in range(X):
            to_mate(c, i).wait_send()
            if i:
                to_far(c, i).wait_send()


def sum_parts(mesh, p):
    T = mesh.shape["tp"]
    X = T // 2
    n, width = p.shape[0], p.shape[1] // T
    nc = 4
    dma = pltpu.SemaphoreType.DMA
    vmem = pl.BlockSpec(memory_space=pltpu.VMEM)
    return pl.pallas_call(
        functools.partial(sum_kernel, X, nc),
        out_shape=jax.ShapeDtypeStruct((n, width), jnp.bfloat16),
        in_specs=[vmem],
        out_specs=vmem,
        scratch_shapes=[pltpu.VMEM((X, n, width), jnp.bfloat16)] * 3 + [dma((X, nc))] * 4,
        compiler_params=pltpu.CompilerParams(
            collective_id=1, has_side_effects=True, vmem_limit_bytes=16 * 1024 * 1024
        ),
        name="sum_parts",
    )(p)


def solution(mesh):
    def on_device(tokens, norm_gain, gate_weight, up_weight, down_weight):
        row_gain = norm_gain[:, None]
        gate_local = (row_gain * gate_weight).astype(jnp.bfloat16)
        up_local = (row_gain * up_weight).astype(jnp.bfloat16)
        down_local = down_weight.astype(jnp.bfloat16)
        wg, wu, wd, hidden = gather(mesh, gate_local, up_local, down_local, tokens)
        part, og, ou, od = layer(mesh, hidden, wg, wu, wd)
        return (sum_parts(mesh, part), og, ou, od)

    return jax.shard_map(
        on_device,
        mesh=mesh,
        in_specs=(P("fs", None), P("fs"), P("fs", "tp"), P("fs", "tp"), P("fs", "tp")),
        out_specs=(P("fs", "tp"), P(None, "tp"), P(None, "tp"), P("tp", None)),
        check_vma=False,
    )
```
